32 devices in a mesh: grp: 2 (over y), sp: 4 (over z), tp: 4 (over x, core).
Axes of the slice: x: 2, y: 2, z: 4, core: 2. Of those that a mesh axis runs over, the one named last changes fastest.
Arguments:
- query_rows: bfloat16 [3072, 2048], P(('grp', 'sp'), 'tp'), parts along dimension 0, may hold values from -6 to 6, as said below
- key_rows: bfloat16 [3072, 1024], P(('grp', 'sp'), 'tp'), parts along dimension 0, may hold values from -6 to 6, as said below
- value_rows: bfloat16 [3072, 1024], P(('grp', 'sp'), 'tp'), parts along dimension 0, may hold values from -15 to 15
- pool_input: bfloat16 [3072, 2048], P(('grp', 'sp'), 'tp'), parts along dimension 0, may hold values from -6 to 6
- log_gate_sums: float32 [3072, 16], P(('grp', 'sp'), 'tp'), parts along dimension 0, as said below
- query_gain: float32 [128], replicated, may hold values from 0.7 to 4.5, as said below
- key_gain: float32 [128], replicated, may hold values from 0.7 to 4.5, as said below
- pool_weight: bfloat16 [8, 256, 256], P('tp'), may hold values from -0.375 to 0.375
- pool_scale: float32 [2048], P('tp'), may hold values from 0.1 to 1.9
- attention_out: bfloat16 [2048, 4096], P('tp'), may hold values from -0.09375 to 0.09375
- pooling_out: bfloat16 [2048, 4096], P('tp'), may hold values from -0.09375 to 0.09375
Outputs:
- mixed_rows: bfloat16 [3072, 4096], P(('grp', 'sp', 'tp')), parts along dimension 0
The draws below stay inside these ranges and needn't reach their ends.
There are 2 independent parts, one for each index of `grp`. The reference program is written for one: setup_inputs(seed, part) draws one part's arguments, and reference() takes and returns one part's arrays. A program takes and returns all parts, laid end to end along the dimension named above; an argument that names none is the same for every part. Nothing has to cross between parts.
Inputs may be any that keep to these rules, and one draw needn't show every extreme that they name: `query_rows`: normal entries; in some rows a query head's entries may equal its key head's entries of an earlier position. `key_rows`: normal entries. `log_gate_sums`: each column never rises from one position to the next. `query_gain`: Positive. `key_gain`: Positive.
All inputs are finite; a program needn't handle non-finite values.
Results may differ from the reference program's by a relative error of at most 0.014.
The reference program's roundings to bfloat16 on the way count: a program that leaves them out, or rounds other values in their place, can miss the bound.
Values may be sent and summed in bfloat16 or wider, within the bound.
A program may use at most 64 MiB of HBM per device.

```python
import math
import jax
import jax.numpy as jnp
from jax import lax

D = 4096
HEAD = 128
QUERY_HEADS = 16
KV_HEADS = 8
POOL_GROUPS = 8
GROUP = 256
MAX_WINDOW = 16
TOK_DEV = 384
SEQUENCE_TOKENS = 1536
ATT_W = 2048
POOL_W = 2048
N_TP = 4


def key_matrix(key):
    matrix = jax.random.normal(jax.random.fold_in(key, 11), (SEQUENCE_TOKENS, KV_HEADS * HEAD), jnp.float32)
    return jnp.clip(matrix, -6.0, 6.0)


def draw_key_rows(key, part):
    return key_matrix(key).astype(jnp.bfloat16)


def draw_query_rows(key, part):
    matrix = jax.random.normal(jax.random.fold_in(key, 17), (SEQUENCE_TOKENS, QUERY_HEADS * HEAD), jnp.float32)
    return jnp.clip(matrix, -6.0, 6.0).astype(jnp.bfloat16)


def gain_draw(key, salt):
    subkey = jax.random.fold_in(key, salt)
    return jax.random.uniform(subkey, (HEAD,), jnp.float32, 0.7, 1.3)


def draw_query_gain(key, part):
    return gain_draw(key, 19)


def draw_key_gain(key, part):
    return gain_draw(key, 23)


def draw_log_gate_sums(key, part):
    ranking = jax.random.permutation(jax.random.fold_in(key, 29), QUERY_HEADS)
    lasting = ranking < QUERY_HEADS // 2
    whole_loss = jax.random.uniform(jax.random.fold_in(key, 31), (QUERY_HEADS,), jnp.float32, 0.3, 0.8)
    forget_span = jax.random.uniform(jax.random.fold_in(key, 37), (QUERY_HEADS,), jnp.float32, 30.0, 100.0)
    baseline_rate = jnp.where(lasting, whole_loss / SEQUENCE_TOKENS, 1.0 / forget_span)
    span_count = SEQUENCE_TOKENS // TOK_DEV
    span_factor = jnp.exp(jax.random.uniform(jax.random.fold_in(key, 41), (span_count, 1), jnp.float32, -0.7, 0.7))
    multiplier = jnp.repeat(span_factor, TOK_DEV, axis=0)
    jaggedness = jax.random.uniform(jax.random.fold_in(key, 43), (SEQUENCE_TOKENS, QUERY_HEADS), jnp.float32, 0.2, 1.8)
    spike_positions = jax.random.randint(jax.random.fold_in(key, 47), (3,), 0, SEQUENCE_TOKENS)
    spike_depth = jax.random.uniform(jax.random.fold_in(key, 53), (3, QUERY_HEADS), jnp.float32, 0.22, 0.69)
    spike_count = (jnp.arange(SEQUENCE_TOKENS)[:, None] == spike_positions[None, :]).astype(jnp.float32)
    spike_events = jnp.dot(spike_count, spike_depth)
    return jnp.cumsum(-(baseline_rate[None, :] * multiplier * jaggedness + spike_events), axis=0)


def level_of(stream_key, shape, split, least, largest):
    gain = 1.0
    for dim, shards_of in split:
        draws = jax.random.uniform(jax.random.fold_in(jax.random.fold_in(stream_key, 6), dim), (shards_of,), jnp.float32, least / len(split), largest / len(split))
        gain = gain * jnp.repeat(jnp.exp(draws), shape[dim] // shards_of).reshape((-1,) + (1,) * (len(shape) - 1 - dim))
    return gain


def bell_draw(stream_key, dims, spread, limit, shards=(), kind=jnp.bfloat16):
    array = jax.random.normal(stream_key, dims, jnp.float32) * spread
    if len(shards) > 0:
        array = level_of(stream_key, dims, shards, -0.22, 0.18) * array
    return jnp.clip(array, min=-limit, max=limit).astype(kind)


def setup_inputs(seed: int = 0, part: int = 0) -> dict:
    streams_of = jax.random.split(jax.random.key(seed), 12)
    part_splits = jax.random.split(jax.random.fold_in(streams_of[11], part), 12)
    return {
        "query_rows": draw_query_rows(jax.random.fold_in(jax.random.fold_in(streams_of[11], part), 71), part),
        "key_rows": draw_key_rows(jax.random.fold_in(jax.random.fold_in(streams_of[11], part), 71), part),
        "value_rows": bell_draw(part_splits[2], (SEQUENCE_TOKENS, KV_HEADS * HEAD), 2.5, 15.0, ((0, 4), (1, 4))),
        "pool_input": bell_draw(part_splits[3], (SEQUENCE_TOKENS, POOL_W), 1.0, 6.0, ((0, 4), (1, 4))),
        "log_gate_sums": draw_log_gate_sums(jax.random.fold_in(jax.random.fold_in(streams_of[11], part), 71), part),
        "query_gain": draw_query_gain(jax.random.fold_in(streams_of[11], 71), part),
        "key_gain": draw_key_gain(jax.random.fold_in(streams_of[11], 71), part),
        "pool_weight": bell_draw(streams_of[7], (POOL_GROUPS, GROUP, GROUP), GROUP ** -0.5, 0.375, ((0, 4),)),
        "pool_scale": jnp.clip(1.0 + 0.18 * jax.random.normal(streams_of[8], (POOL_W,), jnp.float32), 0.1, 1.9),
        "attention_out": bell_draw(streams_of[9], (ATT_W, D), (ATT_W + POOL_W) ** -0.5, 0.09375, ((0, 4),)),
        "pooling_out": bell_draw(streams_of[10], (POOL_W, D), (ATT_W + POOL_W) ** -0.5, 0.09375, ((0, 4),)),
    }


epsilon = 1e-06
masked = -1e+30

def head_norm(row_data, gain_vector, head_count):
    shaped = row_data.astype(jnp.float32).reshape(row_data.shape[0], head_count, -1)
    scaled = shaped * lax.rsqrt(lax.optimization_barrier(jnp.mean(shaped * shaped, axis=-1, keepdims=True)) + epsilon)
    return (scaled * gain_vector).astype(jnp.bfloat16)

def window_means(padded, length, first_pos, windows):
    rim_rows = padded.shape[0] - length
    window_sum = jnp.zeros((length,) + padded.shape[1:], jnp.float32)
    pooled = window_sum
    for lookback in range(rim_rows + 1):
        window_sum = window_sum + padded[rim_rows - lookback:rim_rows - lookback + length]
        window_size = lookback + 1
        if window_size >= 2 and window_size & window_size - 1 == 0:
            pooled = jnp.where((windows == window_size)[None, :, None], window_sum, pooled)
    positions = (first_pos + jnp.arange(length, dtype=jnp.int32)).astype(jnp.float32)
    counts = jnp.minimum(positions[:, None, None] + 1.0, windows.astype(jnp.float32)[None, :, None])
    return pooled / counts - padded[rim_rows:]

def reference(query_rows, key_rows, value_rows, pool_input, log_gate_sums, query_gain, key_gain, pool_weight, pool_scale, attention_out, pooling_out):
    ratio = QUERY_HEADS // KV_HEADS
    queries = head_norm(query_rows, query_gain, QUERY_HEADS).transpose(1, 0, 2)
    normed_keys = jnp.repeat(head_norm(key_rows, key_gain, KV_HEADS), ratio, axis=1).transpose(1, 0, 2)
    values = jnp.repeat(value_rows.reshape(SEQUENCE_TOKENS, KV_HEADS, HEAD), ratio, axis=1).transpose(1, 0, 2)
    gates = log_gate_sums.T
    block_rows = math.gcd(SEQUENCE_TOKENS, 512)
    key_pos = jnp.arange(SEQUENCE_TOKENS, dtype=jnp.int32)

    def attend_head(operands):
        head_query, head_key, head_value, head_gate = operands

        def one_block(block_index):
            first = block_index * block_rows
            block_query = lax.dynamic_slice_in_dim(head_query, first, block_rows, 0)
            block_gate = lax.dynamic_slice_in_dim(head_gate, first, block_rows, 0)
            scores = jnp.dot(block_query, head_key.T, preferred_element_type=jnp.float32)
            scores = scores * (1.0 / math.sqrt(HEAD)) + block_gate[:, None] - head_gate[None, :]
            allowed = key_pos[None, :] <= (first + jnp.arange(block_rows, dtype=jnp.int32))[:, None]
            scores = jnp.where(allowed, scores, masked)
            row_best = lax.optimization_barrier(jnp.max(scores, axis=-1, keepdims=True))
            weights = jnp.where(allowed, jnp.exp(scores - row_best), 0.0)
            weight_sum = lax.optimization_barrier(jnp.sum(weights, axis=-1, keepdims=True))
            summed = jnp.dot(weights.astype(jnp.bfloat16), head_value, preferred_element_type=jnp.float32)
            return (summed / weight_sum).astype(jnp.bfloat16)
        return lax.map(one_block, jnp.arange(SEQUENCE_TOKENS // block_rows, dtype=jnp.int32)).reshape(SEQUENCE_TOKENS, HEAD)
    attended = lax.map(attend_head, (queries, normed_keys, values, gates))
    attended = attended.transpose(1, 0, 2).reshape(SEQUENCE_TOKENS, QUERY_HEADS * HEAD)
    padded = jnp.concatenate([jnp.zeros((MAX_WINDOW - 1, POOL_GROUPS * GROUP), jnp.float32), pool_input.astype(jnp.float32)])
    padded = padded.reshape(SEQUENCE_TOKENS + MAX_WINDOW - 1, POOL_GROUPS, GROUP)
    levels = MAX_WINDOW.bit_length() - 1
    windows = 2 ** (1 + jnp.arange(POOL_GROUPS, dtype=jnp.int32) % levels)
    pooled = window_means(padded, SEQUENCE_TOKENS, 0, windows).astype(jnp.bfloat16)
    mixing = jnp.einsum('tgc,gcd->tgd', pooled.astype(jnp.float32), pool_weight.astype(jnp.float32))
    pool_mixed = (mixing * pool_scale.reshape(POOL_GROUPS, GROUP)).astype(jnp.bfloat16).reshape(SEQUENCE_TOKENS, POOL_GROUPS * GROUP)
    attend_share = QUERY_HEADS * HEAD // N_TP
    pool_share = POOL_GROUPS * GROUP // N_TP
    merged = jnp.zeros((SEQUENCE_TOKENS, D), jnp.float32)
    for device in range(N_TP):
        attend_cols = attended[:, device * attend_share:(device + 1) * attend_share]
        pool_cols = pool_mixed[:, device * pool_share:(device + 1) * pool_share]
        partial_sum = jnp.dot(attend_cols, attention_out[device * attend_share:(device + 1) * attend_share], preferred_element_type=jnp.float32)
        partial_sum = partial_sum + jnp.dot(pool_cols, pooling_out[device * pool_share:(device + 1) * pool_share], preferred_element_type=jnp.float32)
        rounded = lax.optimization_barrier(partial_sum.astype(jnp.bfloat16))
        merged = merged + rounded.astype(jnp.float32)
    return merged.astype(jnp.bfloat16)
```

```python
import functools
import math

import jax
import jax.numpy as jnp
from jax import lax
from jax.experimental import pallas as pl
from jax.experimental.pallas import tpu as pltpu
from jax.sharding import PartitionSpec as P

HEAD = 128
QUERY_HEADS = 16
KV_HEADS = 8
GROUP = 256
MAX_WINDOW = 16
RATIO = QUERY_HEADS // KV_HEADS
RIM = 16
CHUNK = 512

epsilon = 1e-06
masked = -1e30
MESH = pl.DeviceIdType.MESH
f32 = jnp.float32
bf16 = jnp.bfloat16


def normed(rows, gain):
    rows = rows.astype(f32)
    scale = lax.rsqrt(jnp.mean(rows * rows, axis=-1, keepdims=True) + epsilon)
    return (rows * scale * gain).astype(bf16)


def kernel(
    n_sp,
    n_tp,
    q_hbm,
    k_hbm,
    v_hbm,
    p_hbm,
    gates,
    q_gain,
    k_gain,
    pool_weight,
    pool_scale,
    wa_hbm,
    wp_hbm,
    out_hbm,
    q_raw,
    k_raw,
    kv,
    gate_rows,
    qn,
    best,
    sums,
    acc,
    padded,
    act,
    weights,
    part,
    pair_in,
    x_out,
    x_in,
    own,
    out_buf,
    in_sems,
    w_sems,
    kv_send,
    kv_recv,
    rim_sems,
    d_send,
    d_recv,
    x_send,
    x_recv,
    out_sems,
):
    length = q_raw.shape[0]
    kv_here = k_raw.shape[1] // HEAD
    heads = kv_here * RATIO
    group_here = padded.shape[1] // GROUP
    att_w = heads * HEAD
    n_x = n_tp // 2
    rows_out = length // n_tp
    chip_rows = 2 * rows_out
    chunks = weights.shape[0]
    gate_item = 2 * kv_here

    me = lax.axis_index("sp")
    tp = lax.axis_index("tp")
    x = tp // 2
    c = tp % 2
    partner = x * 2 + (1 - c)
    has_next = me < n_sp - 1
    has_prev = me > 0

    def across(dx):
        return lax.rem(x + dx, n_x) * 2 + c

    ins = [
        pltpu.make_async_copy(k_hbm, k_raw, in_sems.at[0]),
        pltpu.make_async_copy(p_hbm, padded.at[pl.ds(RIM, length)], in_sems.at[1]),
        pltpu.make_async_copy(q_hbm, q_raw, in_sems.at[2]),
    ]
    for h in range(kv_here):
        ins.append(
            pltpu.make_async_copy(
                v_hbm.at[:, pl.ds(h * HEAD, HEAD)], kv.at[me, h, 1], in_sems.at[3 + h]
            )
        )
    for copy in ins:
        copy.start()
    loads = []
    for j in range(chunks):
        cols = pl.ds(j * CHUNK, CHUNK)
        loads.append(
            pltpu.make_async_copy(
                wa_hbm.at[:, cols], weights.at[j, pl.ds(0, att_w)], w_sems.at[2 * j]
            )
        )
        loads.append(
            pltpu.make_async_copy(
                wp_hbm.at[:, cols],
                weights.at[j, pl.ds(att_w, weights.shape[1] - att_w)],
                w_sems.at[2 * j + 1],
            )
        )

    barrier = pltpu.get_barrier_semaphore()

    def greet(where):
        pl.semaphore_signal(barrier, inc=1, device_id=where, device_id_type=MESH)

    @pl.when(has_next)
    def _():
        greet({"sp": me + 1})

    @pl.when(has_prev)
    def _():
        greet({"sp": me - 1})

    greet({"tp": partner})
    for dx in range(1, n_x):
        greet({"tp": across(dx)})

    k_scale = k_gain[...]
    q_scale = q_gain[...]
    ins[0].wait()
    for h in range(kv_here):
        kv[me, h, 0] = normed(k_raw[:, h * HEAD : (h + 1) * HEAD], k_scale)
    on_diagonal = lax.broadcasted_iota(jnp.int32, (length, length), 0) == (
        lax.broadcasted_iota(jnp.int32, (length, length), 1)
    )
    for i in range(heads):
        gate_rows[me, pl.ds(i, 1)] = jnp.sum(
            jnp.where(on_diagonal, gates[:, i : i + 1], 0.0), axis=0, keepdims=True
        )
    for copy in ins[3:]:
        copy.wait()
    ins[1].wait()

    pl.semaphore_wait(barrier, n_x + has_next.astype(jnp.int32) + has_prev.astype(jnp.int32))

    after = jnp.minimum(me + 1, n_sp - 1)

    def hand_on(slot, item):
        if item == gate_item:
            block = gate_rows.at[slot]
        else:
            block = kv.at[slot, item // 2, 1 - item % 2]
        return pltpu.make_async_remote_copy(
            src_ref=block,
            dst_ref=block,
            send_sem=kv_send.at[slot, item],
            recv_sem=kv_recv.at[slot, item],
            device_id={"sp": after},
            device_id_type=MESH,
        )

    rim_copy = pltpu.make_async_remote_copy(
        src_ref=padded.at[pl.ds(length, RIM)],
        dst_ref=padded.at[pl.ds(0, RIM)],
        send_sem=rim_sems.at[0],
        recv_sem=rim_sems.at[1],
        device_id={"sp": after},
        device_id_type=MESH,
    )

    @pl.when(has_next)
    def _():
        hand_on(me, gate_item).start()
        for item in range(gate_item):
            hand_on(me, item).start()
        rim_copy.start()

    for copy in loads:
        copy.start()

    ins[2].wait()
    for i in range(heads):
        qn[i] = normed(q_raw[:, i * HEAD : (i + 1) * HEAD], q_scale)

    def score_of(i, slot):
        scores = lax.dot_general(
            qn[i], kv[slot, i // RATIO, 0], (((1,), (1,)), ((), ())), preferred_element_type=f32
        )
        drop = gates[:, i : i + 1] - gate_rows[slot, pl.ds(i, 1)]
        return scores * (1.0 / math.sqrt(HEAD)) + drop

    allowed = lax.broadcasted_iota(jnp.int32, (length, length), 1) <= (
        lax.broadcasted_iota(jnp.int32, (length, length), 0)
    )
    for i in range(heads):
        scores = jnp.where(allowed, score_of(i, me), masked)
        top = jnp.max(scores, axis=-1, keepdims=True)
        shares = jnp.where(allowed, jnp.exp(scores - top), 0.0)
        best[i] = top
        sums[i] = jnp.sum(shares, axis=-1, keepdims=True)
        acc[i] = jnp.dot(shares.astype(bf16), kv[me, i // RATIO, 1], preferred_element_type=f32)

    def attend(i, slot):
        scores = score_of(i, slot)
        old = best[i]
        top = jnp.maximum(old, jnp.max(scores, axis=-1, keepdims=True))
        shares = jnp.exp(scores - top)
        fading = jnp.exp(old - top)
        best[i] = top
        sums[i] = sums[i] * fading + jnp.sum(shares, axis=-1, keepdims=True)
        acc[i] = acc[i] * fading + jnp.dot(
            shares.astype(bf16), kv[slot, i // RATIO, 1], preferred_element_type=f32
        )

    @pl.when(has_prev)
    def _():
        rim_copy.wait_recv()

    @pl.when(jnp.logical_not(has_prev))
    def _():
        padded[pl.ds(0, RIM)] = jnp.zeros((RIM, padded.shape[1]), bf16)

    levels = MAX_WINDOW.bit_length() - 1
    first = me * length
    position = (first + lax.broadcasted_iota(jnp.int32, (length, 1), 0)).astype(f32)
    for g in range(group_here):
        cols = slice(g * GROUP, (g + 1) * GROUP)
        level = (tp * group_here + g) % levels
        rows = padded[:, cols].astype(f32)
        running = rows
        window_sum = None
        for step in range(levels):
            running = running + pltpu.roll(running, 1 << step, 0)
            if window_sum is None:
                window_sum = running
            else:
                window_sum = jnp.where(level >= step, running, window_sum)
        window = lax.shift_left(jnp.int32(2), level).astype(f32)
        counts = jnp.minimum(position + 1.0, window)
        pooled = (window_sum[RIM:] / counts - rows[RIM:]).astype(bf16)
        mixing = jnp.dot(pooled, pool_weight[g], preferred_element_type=f32)
        act[:, att_w + g * GROUP : att_w + (g + 1) * GROUP] = (
            mixing * pool_scale[:, cols]
        ).astype(bf16)

    def one_step(step, carry):
        slot = me - step

        def take(item):
            hand_on(slot, item).wait_recv()

            @pl.when(has_next)
            def _():
                hand_on(slot, item).start()

        take(gate_item)
        for h in range(kv_here):
            take(2 * h)
            take(2 * h + 1)
            for r in range(RATIO):
                attend(h * RATIO + r, slot)
        return carry

    lax.fori_loop(1, me + 1, one_step, 0)
    for i in range(heads):
        act[:, i * HEAD : (i + 1) * HEAD] = (acc[i] / sums[i]).astype(bf16)

    for copy in loads:
        copy.wait()

    def pair_copy(dx, j):
        return pltpu.make_async_remote_copy(
            src_ref=part.at[dx, j, pl.ds(pl.multiple_of((1 - c) * rows_out, 16), rows_out)],
            dst_ref=pair_in.at[dx, j],
            send_sem=d_send.at[dx, j],
            recv_sem=d_recv.at[dx, j],
            device_id={"tp": partner},
            device_id_type=MESH,
        )

    def x_copy(dx, j):
        return pltpu.make_async_remote_copy(
            src_ref=x_out.at[dx - 1, j],
            dst_ref=x_in.at[dx - 1, j],
            send_sem=x_send.at[dx - 1, j],
            recv_sem=x_recv.at[dx - 1, j],
            device_id={"tp": across(dx)},
            device_id_type=MESH,
        )

    def project(dx, j):
        top_row = pl.multiple_of(lax.rem(x + dx, n_x) * chip_rows, 16)
        part[dx, j] = jnp.dot(
            act[pl.ds(top_row, chip_rows)], weights[j], preferred_element_type=f32
        ).astype(bf16)
        pair_copy(dx, j).start()

    def pair_sum(dx, j):
        pair_copy(dx, j).wait_recv()
        mine = part[dx, j, pl.ds(pl.multiple_of(c * rows_out, 16), rows_out)]
        return mine.astype(f32) + pair_in[dx, j].astype(f32)

    for dx in list(range(1, n_x)) + [0]:

        def finish(j, dx=dx):
            total = pair_sum(dx, j)
            if dx == 0:
                own[j] = total
            else:
                x_out[dx - 1, j] = total.astype(bf16)
                x_copy(dx, j).start()

        def one_chunk(j, carry, dx=dx, finish=finish):
            project(dx, j)

            @pl.when(j > 0)
            def _():
                finish(j - 1)

            return carry

        lax.fori_loop(0, chunks, one_chunk, 0)
        finish(chunks - 1)

    def out_copy(j):
        return pltpu.make_async_copy(
            out_buf.at[j],
            out_hbm.at[:, pl.ds(pl.multiple_of(j * CHUNK, CHUNK), CHUNK)],
            out_sems.at[j],
        )

    def last(j, carry):
        total = own[j]
        for dx in range(1, n_x):
            x_copy(dx, j).wait_recv()
            total = total + x_in[dx - 1, j].astype(f32)
        out_buf[j] = total.astype(bf16)
        out_copy(j).start()
        return carry

    lax.fori_loop(0, chunks, last, 0)

    def drain(j, carry):
        out_copy(j).wait()
        for dx in range(n_x):
            pair_copy(dx, j).wait_send()
            if dx:
                x_copy(dx, j).wait_send()
        return carry

    lax.fori_loop(0, chunks, drain, 0)

    @pl.when(has_next)
    def _():
        rim_copy.wait_send()

        def sent(slot, carry):
            for item in range(gate_item + 1):
                hand_on(slot, item).wait_send()
            return carry

        lax.fori_loop(0, me + 1, sent, 0)


def body(n_sp, n_tp, q, k, v, p, gates, q_gain, k_gain, pool_weight, pool_scale, wa, wp):
    length = q.shape[0]
    kv_here = k.shape[1] // HEAD
    heads = kv_here * RATIO
    width = wa.shape[1]
    n_x = n_tp // 2
    rows_out = length // n_tp
    chunks = width // CHUNK
    depth = wa.shape[0] + wp.shape[0]
    items = 2 * kv_here + 1
    dma = pltpu.SemaphoreType.DMA
    hbm = pl.BlockSpec(memory_space=pl.ANY)
    vmem = pl.BlockSpec(memory_space=pltpu.VMEM)
    far = max(n_x - 1, 1)
    return pl.pallas_call(
        functools.partial(kernel, n_sp, n_tp),
        out_shape=jax.ShapeDtypeStruct((rows_out, width), bf16),
        in_specs=[hbm] * 4 + [vmem] * 5 + [hbm] * 2,
        out_specs=hbm,
        scratch_shapes=[
            pltpu.VMEM(q.shape, bf16),
            pltpu.VMEM(k.shape, bf16),
            pltpu.VMEM((n_sp, kv_here, 2, length, HEAD), bf16),
            pltpu.VMEM((n_sp, 8, length), f32),
            pltpu.VMEM((heads, length, HEAD), bf16),
            pltpu.VMEM((heads, length, 1), f32),
            pltpu.VMEM((heads, length, 1), f32),
            pltpu.VMEM((heads, length, HEAD), f32),
            pltpu.VMEM((length + RIM, p.shape[1]), bf16),
            pltpu.VMEM((length, depth), bf16),
            pltpu.VMEM((chunks, depth, CHUNK), bf16),
            pltpu.VMEM((n_x, chunks, 2 * rows_out, CHUNK), bf16),
            pltpu.VMEM((n_x, chunks, rows_out, CHUNK), bf16),
            pltpu.VMEM((far, chunks, rows_out, CHUNK), bf16),
            pltpu.VMEM((far, chunks, rows_out, CHUNK), bf16),
            pltpu.VMEM((chunks, rows_out, CHUNK), f32),
            pltpu.VMEM((chunks, rows_out, CHUNK), bf16),
            dma((3 + kv_here,)),
            dma((2 * chunks,)),
            dma((n_sp, items)),
            dma((n_sp, items)),
            dma((2,)),
            dma((n_x, chunks)),
            dma((n_x, chunks)),
            dma((far, chunks)),
            dma((far, chunks)),
            dma((chunks,)),
        ],
        compiler_params=pltpu.CompilerParams(
            collective_id=0, has_side_effects=True, vmem_limit_bytes=60 * 1024 * 1024
        ),
        name="mixer",
    )(
        q,
        k,
        v,
        p,
        gates,
        q_gain.reshape(1, -1),
        k_gain.reshape(1, -1),
        pool_weight,
        pool_scale.reshape(1, -1),
        wa,
        wp,
    )


def solution(mesh):
    return jax.shard_map(
        functools.partial(body, mesh.shape["sp"], mesh.shape["tp"]),
        mesh=mesh,
        in_specs=(
            P(("grp", "sp"), "tp"),
            P(("grp", "sp"), "tp"),
            P(("grp", "sp"), "tp"),
            P(("grp", "sp"), "tp"),
            P(("grp", "sp"), "tp"),
            P(),
            P(),
            P("tp", None, None),
            P("tp"),
            P("tp", None),
            P("tp", None),
        ),
        out_specs=P(("grp", "sp", "tp"), None),
        check_vma=False,
    )
```

```python
import functools
import math

import jax
import jax.numpy as jnp
from jax import lax
from jax.experimental import pallas as pl
from jax.experimental.pallas import tpu as pltpu
from jax.sharding import PartitionSpec as P

HEAD = 128
QUERY_HEADS = 16
KV_HEADS = 8
GROUP = 256
MAX_WINDOW = 16
RATIO = QUERY_HEADS // KV_HEADS
RIM = 16
CHUNK = 256

epsilon = 1e-06
masked = -1e30
MESH = pl.DeviceIdType.MESH
f32 = jnp.float32
bf16 = jnp.bfloat16


def normed(rows, gain):
    rows = rows.astype(f32)
    scale = lax.rsqrt(jnp.mean(rows * rows, axis=-1, keepdims=True) + epsilon)
    return (rows * scale * gain).astype(bf16)


def kernel(
    n_sp,
    n_tp,
    q_hbm,
    k_hbm,
    v_hbm,
    p_hbm,
    gates,
    q_gain,
    k_gain,
    pool_weight,
    pool_scale,
    wa_hbm,
    wp_hbm,
    out_hbm,
    q_raw,
    k_raw,
    kv,
    gate_rows,
    gate_cols,
    qn,
    best,
    sums,
    acc,
    padded,
    act,
    weights,
    part,
    pair_in,
    x_out,
    x_in,
    own,
    out_buf,
    in_sems,
    w_sems,
    kv_send,
    kv_recv,
    rim_sems,
    d_send,
    d_recv,
    x_send,
    x_recv,
    out_sems,
):
    length = q_raw.shape[0]
    kv_here = k_raw.shape[1] // HEAD
    heads = kv_here * RATIO
    group_here = padded.shape[1] // GROUP
    att_w = heads * HEAD
    n_x = n_tp // 2
    rows_out = length // n_tp
    chip_rows = 2 * rows_out
    chunks = weights.shape[0]
    gate_item = 2 * kv_here

    me = lax.axis_index("sp")
    tp = lax.axis_index("tp")
    x = tp // 2
    c = tp % 2
    partner = x * 2 + (1 - c)
    has_next = me < n_sp - 1
    has_prev = me > 0

    def across(dx):
        return lax.rem(x + dx, n_x) * 2 + c

    ins = [
        pltpu.make_async_copy(k_hbm, k_raw, in_sems.at[0]),
        pltpu.make_async_copy(p_hbm, padded.at[pl.ds(RIM, length)], in_sems.at[1]),
        pltpu.make_async_copy(q_hbm, q_raw, in_sems.at[2]),
    ]
    for h in range(kv_here):
        ins.append(
            pltpu.make_async_copy(
                v_hbm.at[:, pl.ds(h * HEAD, HEAD)], kv.at[me, h, 1], in_sems.at[3 + h]
            )
        )
    for copy in ins:
        copy.start()
    loads = []
    for j in range(chunks):
        cols = pl.ds(j * CHUNK, CHUNK)
        loads.append(
            pltpu.make_async_copy(
                wa_hbm.at[:, cols], weights.at[j, pl.ds(0, att_w)], w_sems.at[2 * j]
            )
        )
        loads.append(
            pltpu.make_async_copy(
                wp_hbm.at[:, cols],
                weights.at[j, pl.ds(att_w, weights.shape[1] - att_w)],
                w_sems.at[2 * j + 1],
            )
        )

    barrier = pltpu.get_barrier_semaphore()

    def greet(where):
        pl.semaphore_signal(barrier, inc=1, device_id=where, device_id_type=MESH)

    @pl.when(has_next)
    def _():
        greet({"sp": me + 1})

    @pl.when(has_prev)
    def _():
        greet({"sp": me - 1})

    greet({"tp": partner})
    for dx in range(1, n_x):
        greet({"tp": across(dx)})

    k_scale = k_gain[...]
    q_scale = q_gain[...]
    ins[0].wait()
    for h in range(kv_here):
        kv[me, h, 0] = normed(k_raw[:, h * HEAD : (h + 1) * HEAD], k_scale)
    for copy in ins[3:]:
        copy.wait()
    ins[1].wait()

    pl.semaphore_wait(barrier, n_x + has_next.astype(jnp.int32) + has_prev.astype(jnp.int32))

    after = jnp.minimum(me + 1, n_sp - 1)

    def hand_on(slot, item, own_gates=False):
        if item == gate_item:
            block = gate_rows.at[slot]
        else:
            block = kv.at[slot, item // 2, item % 2]
        return pltpu.make_async_remote_copy(
            src_ref=gates if own_gates else block,
            dst_ref=block,
            send_sem=kv_send.at[slot, item],
            recv_sem=kv_recv.at[slot, item],
            device_id={"sp": after},
            device_id_type=MESH,
        )

    rim_copy = pltpu.make_async_remote_copy(
        src_ref=padded.at[pl.ds(length, RIM)],
        dst_ref=padded.at[pl.ds(0, RIM)],
        send_sem=rim_sems.at[0],
        recv_sem=rim_sems.at[1],
        device_id={"sp": after},
        device_id_type=MESH,
    )

    @pl.when(has_next)
    def _():
        rim_copy.start()
        hand_on(me, 0).start()
        hand_on(me, gate_item, True).start()
        for item in range(1, gate_item):
            hand_on(me, item).start()

    for copy in loads:
        copy.start()

    ins[2].wait()
    for i in range(heads):
        qn[i] = normed(q_raw[:, i * HEAD : (i + 1) * HEAD], q_scale)

    on_diagonal = lax.broadcasted_iota(jnp.int32, (length, length), 0) == (
        lax.broadcasted_iota(jnp.int32, (length, length), 1)
    )
    for i in range(heads):
        gate_cols[i] = jnp.sum(
            jnp.where(on_diagonal, gates[pl.ds(i, 1)], 0.0), axis=1, keepdims=True
        )

    def score_of(i, slot, key_gates):
        scores = lax.dot_general(
            qn[i], kv[slot, i // RATIO, 0], (((1,), (1,)), ((), ())), preferred_element_type=f32
        )
        drop = gate_cols[i] - key_gates
        return scores * (1.0 / math.sqrt(HEAD)) + drop

    allowed = lax.broadcasted_iota(jnp.int32, (length, length), 1) <= (
        lax.broadcasted_iota(jnp.int32, (length, length), 0)
    )
    for i in range(heads):
        scores = jnp.where(allowed, score_of(i, me, gates[pl.ds(i, 1)]), masked)
        top = jnp.max(scores, axis=-1, keepdims=True)
        shares = jnp.where(allowed, jnp.exp(scores - top), 0.0)
        best[i] = top
        sums[i] = jnp.sum(shares, axis=-1, keepdims=True)
        acc[i] = jnp.dot(shares.astype(bf16), kv[me, i // RATIO, 1], preferred_element_type=f32)

    def one_step(step, carry):
        slot = me - step

        def take(item):
            hand_on(slot, item).wait_recv()

            @pl.when(has_next)
            def _():
                hand_on(slot, item).start()

        take(0)
        take(gate_item)
        for h in range(kv_here):
            if h:
                take(2 * h)
            held = []
            for i in range(h * RATIO, (h + 1) * RATIO):
                scores = score_of(i, slot, gate_rows[slot, pl.ds(i, 1)])
                old = best[i]
                top = jnp.maximum(old, jnp.max(scores, axis=-1, keepdims=True))
                shares = jnp.exp(scores - top)
                fading = jnp.exp(old - top)
                best[i] = top
                sums[i] = sums[i] * fading + jnp.sum(shares, axis=-1, keepdims=True)
                held.append((i, shares.astype(bf16), fading))
            take(2 * h + 1)
            for i, shares, fading in held:
                acc[i] = acc[i] * fading + jnp.dot(
                    shares, kv[slot, h, 1], preferred_element_type=f32
                )
        return carry

    lax.fori_loop(1, jnp.minimum(me, 1) + 1, one_step, 0)

    @pl.when(has_prev)
    def _():
        rim_copy.wait_recv()

    @pl.when(jnp.logical_not(has_prev))
    def _():
        padded[pl.ds(0, RIM)] = jnp.zeros((RIM, padded.shape[1]), bf16)

    levels = MAX_WINDOW.bit_length() - 1
    first = me * length
    position = (first + lax.broadcasted_iota(jnp.int32, (length, 1), 0)).astype(f32)
    for g in range(group_here):
        cols = slice(g * GROUP, (g + 1) * GROUP)
        level = (tp * group_here + g) % levels
        rows = padded[:, cols].astype(f32)
        running = rows
        window_sum = None
        for step in range(levels):
            running = running + pltpu.roll(running, 1 << step, 0)
            if window_sum is None:
                window_sum = running
            else:
                window_sum = jnp.where(level >= step, running, window_sum)
        window = lax.shift_left(jnp.int32(2), level).astype(f32)
        counts = jnp.minimum(position + 1.0, window)
        pooled = (window_sum[RIM:] / counts - rows[RIM:]).astype(bf16)
        mixing = jnp.dot(pooled, pool_weight[g], preferred_element_type=f32)
        act[:, att_w + g * GROUP : att_w + (g + 1) * GROUP] = (
            mixing * pool_scale[:, cols]
        ).astype(bf16)

    lax.fori_loop(2, me + 1, one_step, 0)
    for i in range(heads):
        act[:, i * HEAD : (i + 1) * HEAD] = (acc[i] / sums[i]).astype(bf16)

    for copy in loads:
        copy.wait()

    def pair_copy(dx, j):
        return pltpu.make_async_remote_copy(
            src_ref=part.at[dx, j, pl.ds(pl.multiple_of((1 - c) * rows_out, 16), rows_out)],
            dst_ref=pair_in.at[dx, j],
            send_sem=d_send.at[dx, j],
            recv_sem=d_recv.at[dx, j],
            device_id={"tp": partner},
            device_id_type=MESH,
        )

    def x_copy(dx, j):
        return pltpu.make_async_remote_copy(
            src_ref=x_out.at[dx - 1, j],
            dst_ref=x_in.at[dx - 1, j],
            send_sem=x_send.at[dx - 1, j],
            recv_sem=x_recv.at[dx - 1, j],
            device_id={"tp": across(dx)},
            device_id_type=MESH,
        )

    def project(dx, j):
        top_row = pl.multiple_of(lax.rem(x + dx, n_x) * chip_rows, 16)
        part[dx, j] = jnp.dot(
            act[pl.ds(top_row, chip_rows)], weights[j], preferred_element_type=f32
        ).astype(bf16)
        pair_copy(dx, j).start()

    def pair_sum(dx, j):
        pair_copy(dx, j).wait_recv()
        mine = part[dx, j, pl.ds(pl.multiple_of(c * rows_out, 16), rows_out)]
        return mine.astype(f32) + pair_in[dx, j].astype(f32)

    for dx in list(range(1, n_x)) + [0]:

        def finish(j, dx=dx):
            total = pair_sum(dx, j)
            if dx == 0:
                own[j] = total
            else:
                x_out[dx - 1, j] = total.astype(bf16)
                x_copy(dx, j).start()

        def one_chunk(j, carry, dx=dx, finish=finish):
            project(dx, j)

            @pl.when(j > 0)
            def _():
                finish(j - 1)

            return carry

        lax.fori_loop(0, chunks, one_chunk, 0)
        finish(chunks - 1)

    def out_copy(j):
        return pltpu.make_async_copy(
            out_buf.at[j],
            out_hbm.at[:, pl.ds(pl.multiple_of(j * CHUNK, CHUNK), CHUNK)],
            out_sems.at[j],
        )

    def last(j, carry):
        total = own[j]
        for dx in range(1, n_x):
            x_copy(dx, j).wait_recv()
            total = total + x_in[dx - 1, j].astype(f32)
        out_buf[j] = total.astype(bf16)
        out_copy(j).start()
        return carry

    lax.fori_loop(0, chunks, last, 0)

    def drain(j, carry):
        out_copy(j).wait()
        for dx in range(n_x):
            pair_copy(dx, j).wait_send()
            if dx:
                x_copy(dx, j).wait_send()
        return carry

    lax.fori_loop(0, chunks, drain, 0)

    @pl.when(has_next)
    def _():
        rim_copy.wait_send()

        def sent(slot, carry):
            for item in range(gate_item + 1):
                hand_on(slot, item).wait_send()
            return carry

        lax.fori_loop(0, me + 1, sent, 0)


def body(n_sp, n_tp, q, k, v, p, gates, q_gain, k_gain, pool_weight, pool_scale, wa, wp):
    length = q.shape[0]
    kv_here = k.shape[1] // HEAD
    heads = kv_here * RATIO
    width = wa.shape[1]
    n_x = n_tp // 2
    rows_out = length // n_tp
    chunks = width // CHUNK
    depth = wa.shape[0] + wp.shape[0]
    items = 2 * kv_here + 1
    dma = pltpu.SemaphoreType.DMA
    hbm = pl.BlockSpec(memory_space=pl.ANY)
    vmem = pl.BlockSpec(memory_space=pltpu.VMEM)
    far = max(n_x - 1, 1)
    return pl.pallas_call(
        functools.partial(kernel, n_sp, n_tp),
        out_shape=jax.ShapeDtypeStruct((rows_out, width), bf16),
        in_specs=[hbm] * 4 + [vmem] * 5 + [hbm] * 2,
        out_specs=hbm,
        scratch_shapes=[
            pltpu.VMEM(q.shape, bf16),
            pltpu.VMEM(k.shape, bf16),
            pltpu.VMEM((n_sp, kv_here, 2, length, HEAD), bf16),
            pltpu.VMEM((n_sp, heads, length), f32),
            pltpu.VMEM((heads, length, 1), f32),
            pltpu.VMEM((heads, length, HEAD), bf16),
            pltpu.VMEM((heads, length, 1), f32),
            pltpu.VMEM((heads, length, 1), f32),
            pltpu.VMEM((heads, length, HEAD), f32),
            pltpu.VMEM((length + RIM, p.shape[1]), bf16),
            pltpu.VMEM((length, depth), bf16),
            pltpu.VMEM((chunks, depth, CHUNK), bf16),
            pltpu.VMEM((n_x, chunks, 2 * rows_out, CHUNK), bf16),
            pltpu.VMEM((n_x, chunks, rows_out, CHUNK), bf16),
            pltpu.VMEM((far, chunks, rows_out, CHUNK), bf16),
            pltpu.VMEM((far, chunks, rows_out, CHUNK), bf16),
            pltpu.VMEM((chunks, rows_out, CHUNK), f32),
            pltpu.VMEM((chunks, rows_out, CHUNK), bf16),
            dma((3 + kv_here,)),
            dma((2 * chunks,)),
            dma((n_sp, items)),
            dma((n_sp, items)),
            dma((2,)),
            dma((n_x, chunks)),
            dma((n_x, chunks)),
            dma((far, chunks)),
            dma((far, chunks)),
            dma((chunks,)),
        ],
        compiler_params=pltpu.CompilerParams(
            collective_id=0, has_side_effects=True, vmem_limit_bytes=60 * 1024 * 1024
        ),
        name="mixer",
    )(
        q,
        k,
        v,
        p,
        gates.T,
        q_gain.reshape(1, -1),
        k_gain.reshape(1, -1),
        pool_weight,
        pool_scale.reshape(1, -1),
        wa,
        wp,
    )


def solution(mesh):
    return jax.shard_map(
        functools.partial(body, mesh.shape["sp"], mesh.shape["tp"]),
        mesh=mesh,
        in_specs=(
            P(("grp", "sp"), "tp"),
            P(("grp", "sp"), "tp"),
            P(("grp", "sp"), "tp"),
            P(("grp", "sp"), "tp"),
            P(("grp", "sp"), "tp"),
            P(),
            P(),
            P("tp", None, None),
            P("tp"),
            P("tp", None),
            P("tp", None),
        ),
        out_specs=P(("grp", "sp", "tp"), None),
        check_vma=False,
    )
```

```python
import functools
import math

import jax
import jax.numpy as jnp
from jax import lax
from jax.experimental import pallas as pl
from jax.experimental.pallas import tpu as pltpu
from jax.sharding import PartitionSpec as P

HEAD = 128
QUERY_HEADS = 16
KV_HEADS = 8
GROUP = 256
MAX_WINDOW = 16
RATIO = QUERY_HEADS // KV_HEADS
RIM = 16
CHUNK = 256

epsilon = 1e-06
masked = -1e30
MESH = pl.DeviceIdType.MESH
f32 = jnp.float32
bf16 = jnp.bfloat16


def normed(rows, gain):
    rows = rows.astype(f32)
    scale = lax.rsqrt(jnp.mean(rows * rows, axis=-1, keepdims=True) + epsilon)
    return (rows * scale * gain).astype(bf16)


def kernel(
    n_sp,
    n_tp,
    q_hbm,
    k_hbm,
    v_hbm,
    p_hbm,
    gates,
    q_gain,
    k_gain,
    pool_weight,
    pool_scale,
    wa_hbm,
    wp_hbm,
    out_hbm,
    q_raw,
    k_raw,
    kv,
    gate_rows,
    gate_cols,
    qn,
    best,
    sums,
    acc,
    padded,
    act,
    weights,
    part,
    pair_in,
    x_out,
    x_in,
    own,
    out_buf,
    relay_in,
    relay_mid,
    in_sems,
    w_sems,
    kv_send,
    kv_recv,
    rim_sems,
    d_send,
    d_recv,
    x_send,
    x_recv,
    relay_recv,
    mid_send,
    mid_recv,
    back_send,
    out_sems,
):
    length = q_raw.shape[0]
    kv_here = k_raw.shape[1] // HEAD
    heads = kv_here * RATIO
    group_here = padded.shape[1] // GROUP
    att_w = heads * HEAD
    n_x = n_tp // 2
    rows_out = length // n_tp
    chip_rows = 2 * rows_out
    chunks = weights.shape[0]
    gate_item = 2 * kv_here
    relayed = relay_in.shape[1]

    me = lax.axis_index("sp")
    tp = lax.axis_index("tp")
    x = tp // 2
    c = tp % 2
    partner = x * 2 + (1 - c)
    has_next = me < n_sp - 1
    has_prev = me > 0
    relay_at = max(n_sp - 3, 0)
    by_relay = jnp.logical_and(me == n_sp - 1, n_sp >= 3)
    is_relay = jnp.logical_and(me == n_sp - 3, n_sp >= 3)

    def across(dx):
        return lax.rem(x + dx, n_x) * 2 + c

    ins = [
        pltpu.make_async_copy(k_hbm, k_raw, in_sems.at[0]),
        pltpu.make_async_copy(p_hbm, padded.at[pl.ds(RIM, length)], in_sems.at[1]),
        pltpu.make_async_copy(q_hbm, q_raw, in_sems.at[2]),
    ]
    for h in range(kv_here):
        ins.append(
            pltpu.make_async_copy(
                v_hbm.at[:, pl.ds(h * HEAD, HEAD)], kv.at[me, h, 1], in_sems.at[3 + h]
            )
        )
    for copy in ins:
        copy.start()
    loads = []
    for j in range(chunks):
        cols = pl.ds(j * CHUNK, CHUNK)
        loads.append(
            pltpu.make_async_copy(
                wa_hbm.at[:, cols], weights.at[j, pl.ds(0, att_w)], w_sems.at[2 * j]
            )
        )
        loads.append(
            pltpu.make_async_copy(
                wp_hbm.at[:, cols],
                weights.at[j, pl.ds(att_w, weights.shape[1] - att_w)],
                w_sems.at[2 * j + 1],
            )
        )

    barrier = pltpu.get_barrier_semaphore()

    def greet(where):
        pl.semaphore_signal(barrier, inc=1, device_id=where, device_id_type=MESH)

    @pl.when(has_next)
    def _():
        greet({"sp": me + 1})

    @pl.when(has_prev)
    def _():
        greet({"sp": me - 1})

    @pl.when(by_relay)
    def _():
        greet({"sp": relay_at})

    @pl.when(is_relay)
    def _():
        greet({"sp": n_sp - 1})

    greet({"tp": partner})
    for dx in range(1, n_x):
        greet({"tp": across(dx)})

    k_scale = k_gain[...]
    q_scale = q_gain[...]
    ins[0].wait()
    for h in range(kv_here):
        kv[me, h, 0] = normed(k_raw[:, h * HEAD : (h + 1) * HEAD], k_scale)
    for copy in ins[3:]:
        copy.wait()
    ins[1].wait()

    peers = n_x
    for linked in (has_next, has_prev, by_relay, is_relay):
        peers = peers + linked.astype(jnp.int32)
    pl.semaphore_wait(barrier, peers)

    after = jnp.minimum(me + 1, n_sp - 1)

    def hand_on(slot, item, own_gates=False):
        if item == gate_item:
            block = gate_rows.at[slot]
        else:
            block = kv.at[slot, item // 2, item % 2]
        return pltpu.make_async_remote_copy(
            src_ref=gates if own_gates else block,
            dst_ref=block,
            send_sem=kv_send.at[slot, item],
            recv_sem=kv_recv.at[slot, item],
            device_id={"sp": after},
            device_id_type=MESH,
        )

    rim_copy = pltpu.make_async_remote_copy(
        src_ref=padded.at[pl.ds(length, RIM)],
        dst_ref=padded.at[pl.ds(0, RIM)],
        send_sem=rim_sems.at[0],
        recv_sem=rim_sems.at[1],
        device_id={"sp": after},
        device_id_type=MESH,
    )

    @pl.when(has_next)
    def _():
        rim_copy.start()
        hand_on(me, 0).start()
        hand_on(me, gate_item, True).start()
        for item in range(1, gate_item):
            hand_on(me, item).start()

    for copy in loads:
        copy.start()

    ins[2].wait()
    for i in range(heads):
        qn[i] = normed(q_raw[:, i * HEAD : (i + 1) * HEAD], q_scale)

    on_diagonal = lax.broadcasted_iota(jnp.int32, (length, length), 0) == (
        lax.broadcasted_iota(jnp.int32, (length, length), 1)
    )
    for i in range(heads):
        gate_cols[i] = jnp.sum(
            jnp.where(on_diagonal, gates[pl.ds(i, 1)], 0.0), axis=1, keepdims=True
        )

    def score_of(i, slot, key_gates):
        scores = lax.dot_general(
            qn[i], kv[slot, i // RATIO, 0], (((1,), (1,)), ((), ())), preferred_element_type=f32
        )
        drop = gate_cols[i] - key_gates
        return scores * (1.0 / math.sqrt(HEAD)) + drop

    allowed = lax.broadcasted_iota(jnp.int32, (length, length), 1) <= (
        lax.broadcasted_iota(jnp.int32, (length, length), 0)
    )
    for i in range(heads):
        scores = jnp.where(allowed, score_of(i, me, gates[pl.ds(i, 1)]), masked)
        top = jnp.max(scores, axis=-1, keepdims=True)
        shares = jnp.where(allowed, jnp.exp(scores - top), 0.0)
        best[i] = top
        sums[i] = jnp.sum(shares, axis=-1, keepdims=True)
        acc[i] = jnp.dot(shares.astype(bf16), kv[me, i // RATIO, 1], preferred_element_type=f32)

    def one_step(step, carry):
        slot = me - step

        def take(item):
            hand_on(slot, item).wait_recv()

            @pl.when(has_next)
            def _():
                hand_on(slot, item).start()

        take(0)
        take(gate_item)
        for h in range(kv_here):
            if h:
                take(2 * h)
            held = []
            for i in range(h * RATIO, (h + 1) * RATIO):
                scores = score_of(i, slot, gate_rows[slot, pl.ds(i, 1)])
                old = best[i]
                top = jnp.maximum(old, jnp.max(scores, axis=-1, keepdims=True))
                shares = jnp.exp(scores - top)
                fading = jnp.exp(old - top)
                best[i] = top
                sums[i] = sums[i] * fading + jnp.sum(shares, axis=-1, keepdims=True)
                held.append((i, shares.astype(bf16), fading))
            take(2 * h + 1)
            for i, shares, fading in held:
                acc[i] = acc[i] * fading + jnp.dot(
                    shares, kv[slot, h, 1], preferred_element_type=f32
                )
        return carry

    lax.fori_loop(1, jnp.minimum(me, 1) + 1, one_step, 0)

    @pl.when(has_prev)
    def _():
        rim_copy.wait_recv()

    @pl.when(jnp.logical_not(has_prev))
    def _():
        padded[pl.ds(0, RIM)] = jnp.zeros((RIM, padded.shape[1]), bf16)

    levels = MAX_WINDOW.bit_length() - 1
    first = me * length
    position = (first + lax.broadcasted_iota(jnp.int32, (length, 1), 0)).astype(f32)
    for g in range(group_here):
        cols = slice(g * GROUP, (g + 1) * GROUP)
        level = (tp * group_here + g) % levels
        rows = padded[:, cols].astype(f32)
        running = rows
        window_sum = None
        for step in range(levels):
            running = running + pltpu.roll(running, 1 << step, 0)
            if window_sum is None:
                window_sum = running
            else:
                window_sum = jnp.where(level >= step, running, window_sum)
        window = lax.shift_left(jnp.int32(2), level).astype(f32)
        counts = jnp.minimum(position + 1.0, window)
        pooled = (window_sum[RIM:] / counts - rows[RIM:]).astype(bf16)
        mixing = jnp.dot(pooled, pool_weight[g], preferred_element_type=f32)
        act[:, att_w + g * GROUP : att_w + (g + 1) * GROUP] = (
            mixing * pool_scale[:, cols]
        ).astype(bf16)

    lax.fori_loop(2, me + 1, one_step, 0)
    for i in range(heads):
        act[:, i * HEAD : (i + 1) * HEAD] = (acc[i] / sums[i]).astype(bf16)

    for copy in loads:
        copy.wait()

    def pair_copy(dx, j):
        return pltpu.make_async_remote_copy(
            src_ref=part.at[dx, j, pl.ds(pl.multiple_of((1 - c) * rows_out, 16), rows_out)],
            dst_ref=pair_in.at[dx, j],
            send_sem=d_send.at[dx, j],
            recv_sem=d_recv.at[dx, j],
            device_id={"tp": partner},
            device_id_type=MESH,
        )

    def x_copy(dx, j):
        return pltpu.make_async_remote_copy(
            src_ref=x_out.at[dx - 1, j],
            dst_ref=x_in.at[dx - 1, j],
            send_sem=x_send.at[dx - 1, j],
            recv_sem=x_recv.at[dx - 1, j],
            device_id={"tp": across(dx)},
            device_id_type=MESH,
        )

    def to_relay(dx, r):
        return pltpu.make_async_remote_copy(
            src_ref=x_out.at[dx - 1, 2 * r + 1],
            dst_ref=relay_in.at[dx - 1, r],
            send_sem=x_send.at[dx - 1, 2 * r + 1],
            recv_sem=relay_recv.at[dx - 1, r],
            device_id={"sp": relay_at},
            device_id_type=MESH,
        )

    def at_relay(dx, r):
        return pltpu.make_async_remote_copy(
            src_ref=relay_in.at[dx - 1, r],
            dst_ref=relay_mid.at[dx - 1, r],
            send_sem=mid_send.at[dx - 1, r],
            recv_sem=mid_recv.at[dx - 1, r],
            device_id={"tp": across(dx)},
            device_id_type=MESH,
        )

    def from_relay(dx, r):
        return pltpu.make_async_remote_copy(
            src_ref=relay_mid.at[dx - 1, r],
            dst_ref=x_in.at[dx - 1, 2 * r + 1],
            send_sem=back_send.at[dx - 1, r],
            recv_sem=x_recv.at[dx - 1, 2 * r + 1],
            device_id={"sp": n_sp - 1},
            device_id_type=MESH,
        )

    def project(dx, j):
        top_row = pl.multiple_of(lax.rem(x + dx, n_x) * chip_rows, 16)
        part[dx, j] = jnp.dot(
            act[pl.ds(top_row, chip_rows)], weights[j], preferred_element_type=f32
        ).astype(bf16)
        pair_copy(dx, j).start()

    def pair_sum(dx, j):
        pair_copy(dx, j).wait_recv()
        mine = part[dx, j, pl.ds(pl.multiple_of(c * rows_out, 16), rows_out)]
        return mine.astype(f32) + pair_in[dx, j].astype(f32)

    for dx in list(range(1, n_x)) + [0]:

        def finish(j, dx=dx):
            total = pair_sum(dx, j)
            if dx == 0:
                own[j] = total
            else:
                x_out[dx - 1, j] = total.astype(bf16)
                detour = jnp.logical_and(
                    by_relay, jnp.logical_and(lax.rem(j, 2) == 1, j < 2 * relayed)
                )

                @pl.when(detour)
                def _():
                    to_relay(dx, j // 2).start()

                @pl.when(jnp.logical_not(detour))
                def _():
                    x_copy(dx, j).start()

        def one_chunk(j, carry, dx=dx, finish=finish):
            project(dx, j)

            @pl.when(j > 0)
            def _():
                finish(j - 1)

            return carry

        lax.fori_loop(0, chunks, one_chunk, 0)
        finish(jnp.int32(chunks - 1))

    def out_copy(j):
        return pltpu.make_async_copy(
            out_buf.at[j],
            out_hbm.at[:, pl.ds(pl.multiple_of(j * CHUNK, CHUNK), CHUNK)],
            out_sems.at[j],
        )

    def last(j, carry):
        total = own[j]
        for dx in range(1, n_x):
            x_copy(dx, j).wait_recv()
            total = total + x_in[dx - 1, j].astype(f32)
        out_buf[j] = total.astype(bf16)
        out_copy(j).start()
        return carry

    lax.fori_loop(0, chunks, last, 0)

    @pl.when(is_relay)
    def _():
        lag = 2
        for r in range(relayed + lag):
            for dx in range(1, n_x):
                if r < relayed:
                    to_relay(dx, r).wait_recv()
                    at_relay(dx, r).start()
                if r >= lag:
                    at_relay(dx, r - lag).wait_recv()
                    from_relay(dx, r - lag).start()
        for r in range(relayed):
            for dx in range(1, n_x):
                at_relay(dx, r).wait_send()
                from_relay(dx, r).wait_send()

    def drain(j, carry):
        out_copy(j).wait()
        for dx in range(n_x):
            pair_copy(dx, j).wait_send()
            if dx:
                x_copy(dx, j).wait_send()
        return carry

    lax.fori_loop(0, chunks, drain, 0)

    @pl.when(has_next)
    def _():
        rim_copy.wait_send()

        def sent(slot, carry):
            for item in range(gate_item + 1):
                hand_on(slot, item).wait_send()
            return carry

        lax.fori_loop(0, me + 1, sent, 0)


def body(n_sp, n_tp, q, k, v, p, gates, q_gain, k_gain, pool_weight, pool_scale, wa, wp):
    length = q.shape[0]
    kv_here = k.shape[1] // HEAD
    heads = kv_here * RATIO
    width = wa.shape[1]
    n_x = n_tp // 2
    rows_out = length // n_tp
    chunks = width // CHUNK
    depth = wa.shape[0] + wp.shape[0]
    items = 2 * kv_here + 1
    dma = pltpu.SemaphoreType.DMA
    hbm = pl.BlockSpec(memory_space=pl.ANY)
    vmem = pl.BlockSpec(memory_space=pltpu.VMEM)
    far = max(n_x - 1, 1)
    return pl.pallas_call(
        functools.partial(kernel, n_sp, n_tp),
        out_shape=jax.ShapeDtypeStruct((rows_out, width), bf16),
        in_specs=[hbm] * 4 + [vmem] * 5 + [hbm] * 2,
        out_specs=hbm,
        scratch_shapes=[
            pltpu.VMEM(q.shape, bf16),
            pltpu.VMEM(k.shape, bf16),
            pltpu.VMEM((n_sp, kv_here, 2, length, HEAD), bf16),
            pltpu.VMEM((n_sp, heads, length), f32),
            pltpu.VMEM((heads, length, 1), f32),
            pltpu.VMEM((heads, length, HEAD), bf16),
            pltpu.VMEM((heads, length, 1), f32),
            pltpu.VMEM((heads, length, 1), f32),
            pltpu.VMEM((heads, length, HEAD), f32),
            pltpu.VMEM((length + RIM, p.shape[1]), bf16),
            pltpu.VMEM((length, depth), bf16),
            pltpu.VMEM((chunks, depth, CHUNK), bf16),
            pltpu.VMEM((n_x, chunks, 2 * rows_out, CHUNK), bf16),
            pltpu.VMEM((n_x, chunks, rows_out, CHUNK), bf16),
            pltpu.VMEM((far, chunks, rows_out, CHUNK), bf16),
            pltpu.VMEM((far, chunks, rows_out, CHUNK), bf16),
            pltpu.VMEM((chunks, rows_out, CHUNK), f32),
            pltpu.VMEM((chunks, rows_out, CHUNK), bf16),
            pltpu.VMEM((far, max(chunks // 4, 1), rows_out, CHUNK), bf16),
            pltpu.VMEM((far, max(chunks // 4, 1), rows_out, CHUNK), bf16),
            dma((3 + kv_here,)),
            dma((2 * chunks,)),
            dma((n_sp, items)),
            dma((n_sp, items)),
            dma((2,)),
            dma((n_x, chunks)),
            dma((n_x, chunks)),
            dma((far, chunks)),
            dma((far, chunks)),
            dma((far, max(chunks // 4, 1))),
            dma((far, max(chunks // 4, 1))),
            dma((far, max(chunks // 4, 1))),
            dma((far, max(chunks // 4, 1))),
            dma((chunks,)),
        ],
        compiler_params=pltpu.CompilerParams(
            collective_id=0, has_side_effects=True, vmem_limit_bytes=60 * 1024 * 1024
        ),
        name="mixer",
    )(
        q,
        k,
        v,
        p,
        gates.T,
        q_gain.reshape(1, -1),
        k_gain.reshape(1, -1),
        pool_weight,
        pool_scale.reshape(1, -1),
        wa,
        wp,
    )


def solution(mesh):
    return jax.shard_map(
        functools.partial(body, mesh.shape["sp"], mesh.shape["tp"]),
        mesh=mesh,
        in_specs=(
            P(("grp", "sp"), "tp"),
            P(("grp", "sp"), "tp"),
            P(("grp", "sp"), "tp"),
            P(("grp", "sp"), "tp"),
            P(("grp", "sp"), "tp"),
            P(),
            P(),
            P("tp", None, None),
            P("tp"),
            P("tp", None),
            P("tp", None),
        ),
        out_specs=P(("grp", "sp", "tp"), None),
        check_vma=False,
    )
```

```python
import functools
import math

import jax
import jax.numpy as jnp
from jax import lax
from jax.experimental import pallas as pl
from jax.experimental.pallas import tpu as pltpu
from jax.sharding import PartitionSpec as P

HEAD = 128
QUERY_HEADS = 16
KV_HEADS = 8
GROUP = 256
MAX_WINDOW = 16
RATIO = QUERY_HEADS // KV_HEADS
RIM = 16
CHUNK = 256

epsilon = 1e-06
masked = -1e30
MESH = pl.DeviceIdType.MESH
f32 = jnp.float32
bf16 = jnp.bfloat16


def normed(rows, gain):
    rows = rows.astype(f32)
    scale = lax.rsqrt(jnp.mean(rows * rows, axis=-1, keepdims=True) + epsilon)
    return (rows * scale * gain).astype(bf16)


def kernel(
    n_sp,
    n_tp,
    q_hbm,
    k_hbm,
    v_hbm,
    p_hbm,
    gates,
    q_gain,
    k_gain,
    pool_weight,
    pool_scale,
    wa_hbm,
    wp_hbm,
    out_hbm,
    q_raw,
    k_raw,
    kv,
    gate_rows,
    gate_cols,
    qn,
    best,
    sums,
    acc,
    padded,
    act,
    weights,
    part,
    pair_in,
    x_out,
    x_in,
    own,
    out_buf,
    relay_in,
    relay_mid,
    in_sems,
    w_sems,
    kv_send,
    kv_recv,
    rim_sems,
    d_send,
    d_recv,
    x_send,
    x_recv,
    relay_recv,
    mid_send,
    mid_recv,
    back_send,
    out_sems,
):
    length = q_raw.shape[0]
    kv_here = k_raw.shape[1] // HEAD
    heads = kv_here * RATIO
    group_here = padded.shape[1] // GROUP
    att_w = heads * HEAD
    n_x = n_tp // 2
    rows_out = length // n_tp
    chunks = weights.shape[0]
    gate_item = 2 * kv_here
    relayed = relay_in.shape[1]

    me = lax.axis_index("sp")
    tp = lax.axis_index("tp")
    x = tp // 2
    c = tp % 2
    partner = x * 2 + (1 - c)
    has_next = me < n_sp - 1
    has_prev = me > 0
    relay_at = max(n_sp - 3, 0)
    by_relay = jnp.logical_and(me == n_sp - 1, n_sp >= 3)
    is_relay = jnp.logical_and(me == n_sp - 3, n_sp >= 3)

    def across(dx):
        return lax.rem(x + dx, n_x) * 2 + c

    ins = [
        pltpu.make_async_copy(k_hbm, k_raw, in_sems.at[0]),
        pltpu.make_async_copy(p_hbm, padded.at[pl.ds(RIM, length)], in_sems.at[1]),
        pltpu.make_async_copy(q_hbm, q_raw, in_sems.at[2]),
    ]
    for h in range(kv_here):
        ins.append(
            pltpu.make_async_copy(
                v_hbm.at[:, pl.ds(h * HEAD, HEAD)], kv.at[me, h, 1], in_sems.at[3 + h]
            )
        )
    for copy in ins:
        copy.start()
    loads = []
    for j in range(chunks):
        cols = pl.ds(j * CHUNK, CHUNK)
        loads.append(
            pltpu.make_async_copy(
                wa_hbm.at[:, cols], weights.at[j, pl.ds(0, att_w)], w_sems.at[2 * j]
            )
        )
        loads.append(
            pltpu.make_async_copy(
                wp_hbm.at[:, cols],
                weights.at[j, pl.ds(att_w, weights.shape[1] - att_w)],
                w_sems.at[2 * j + 1],
            )
        )

    barrier = pltpu.get_barrier_semaphore()

    def greet(where):
        pl.semaphore_signal(barrier, inc=1, device_id=where, device_id_type=MESH)

    @pl.when(has_next)
    def _():
        greet({"sp": me + 1})

    @pl.when(has_prev)
    def _():
        greet({"sp": me - 1})

    @pl.when(by_relay)
    def _():
        greet({"sp": relay_at})

    @pl.when(is_relay)
    def _():
        greet({"sp": n_sp - 1})

    greet({"tp": partner})
    for dx in range(1, n_x):
        greet({"tp": across(dx)})

    k_scale = k_gain[...]
    q_scale = q_gain[...]
    ins[0].wait()
    for h in range(kv_here):
        kv[me, h, 0] = normed(k_raw[:, h * HEAD : (h + 1) * HEAD], k_scale)
    for copy in ins[3:]:
        copy.wait()
    ins[1].wait()

    peers = n_x
    for linked in (has_next, has_prev, by_relay, is_relay):
        peers = peers + linked.astype(jnp.int32)
    pl.semaphore_wait(barrier, peers)

    after = jnp.minimum(me + 1, n_sp - 1)

    def hand_on(slot, item, own_gates=False):
        if item == gate_item:
            block = gate_rows.at[slot]
        else:
            block = kv.at[slot, item // 2, item % 2]
        return pltpu.make_async_remote_copy(
            src_ref=gates if own_gates else block,
            dst_ref=block,
            send_sem=kv_send.at[slot, item],
            recv_sem=kv_recv.at[slot, item],
            device_id={"sp": after},
            device_id_type=MESH,
        )

    rim_copy = pltpu.make_async_remote_copy(
        src_ref=padded.at[pl.ds(length, RIM)],
        dst_ref=padded.at[pl.ds(0, RIM)],
        send_sem=rim_sems.at[0],
        recv_sem=rim_sems.at[1],
        device_id={"sp": after},
        device_id_type=MESH,
    )

    @pl.when(has_next)
    def _():
        rim_copy.start()
        hand_on(me, 0).start()
        hand_on(me, gate_item, True).start()
        for item in range(1, gate_item):
            hand_on(me, item).start()

    for copy in loads:
        copy.start()

    ins[2].wait()
    for i in range(heads):
        qn[i] = normed(q_raw[:, i * HEAD : (i + 1) * HEAD], q_scale)

    on_diagonal = lax.broadcasted_iota(jnp.int32, (length, length), 0) == (
        lax.broadcasted_iota(jnp.int32, (length, length), 1)
    )
    for i in range(heads):
        gate_cols[i] = jnp.sum(
            jnp.where(on_diagonal, gates[pl.ds(i, 1)], 0.0), axis=1, keepdims=True
        )

    def score_of(i, slot, key_gates):
        scores = lax.dot_general(
            qn[i], kv[slot, i // RATIO, 0], (((1,), (1,)), ((), ())), preferred_element_type=f32
        )
        drop = gate_cols[i] - key_gates
        return scores * (1.0 / math.sqrt(HEAD)) + drop

    allowed = lax.broadcasted_iota(jnp.int32, (length, length), 1) <= (
        lax.broadcasted_iota(jnp.int32, (length, length), 0)
    )
    for i in range(heads):
        scores = jnp.where(allowed, score_of(i, me, gates[pl.ds(i, 1)]), masked)
        top = jnp.max(scores, axis=-1, keepdims=True)
        shares = jnp.where(allowed, jnp.exp(scores - top), 0.0)
        best[i] = top
        sums[i] = jnp.sum(shares, axis=-1, keepdims=True)
        acc[i] = jnp.dot(shares.astype(bf16), kv[me, i // RATIO, 1], preferred_element_type=f32)

    def one_step(step, carry):
        slot = me - step

        def take(item):
            hand_on(slot, item).wait_recv()

            @pl.when(has_next)
            def _():
                hand_on(slot, item).start()

        take(0)
        take(gate_item)
        for h in range(kv_here):
            if h:
                take(2 * h)
            held = []
            for i in range(h * RATIO, (h + 1) * RATIO):
                scores = score_of(i, slot, gate_rows[slot, pl.ds(i, 1)])
                old = best[i]
                top = jnp.maximum(old, jnp.max(scores, axis=-1, keepdims=True))
                shares = jnp.exp(scores - top)
                fading = jnp.exp(old - top)
                best[i] = top
                sums[i] = sums[i] * fading + jnp.sum(shares, axis=-1, keepdims=True)
                held.append((i, shares.astype(bf16), fading))
            take(2 * h + 1)
            for i, shares, fading in held:
                acc[i] = acc[i] * fading + jnp.dot(
                    shares, kv[slot, h, 1], preferred_element_type=f32
                )
        return carry

    lax.fori_loop(1, jnp.minimum(me, 1) + 1, one_step, 0)

    @pl.when(has_prev)
    def _():
        rim_copy.wait_recv()

    @pl.when(jnp.logical_not(has_prev))
    def _():
        padded[pl.ds(0, RIM)] = jnp.zeros((RIM, padded.shape[1]), bf16)

    levels = MAX_WINDOW.bit_length() - 1
    first = me * length
    position = (first + lax.broadcasted_iota(jnp.int32, (length, 1), 0)).astype(f32)
    for g in range(group_here):
        cols = slice(g * GROUP, (g + 1) * GROUP)
        level = (tp * group_here + g) % levels
        rows = padded[:, cols].astype(f32)
        running = rows
        window_sum = None
        for step in range(levels):
            running = running + pltpu.roll(running, 1 << step, 0)
            if window_sum is None:
                window_sum = running
            else:
                window_sum = jnp.where(level >= step, running, window_sum)
        window = lax.shift_left(jnp.int32(2), level).astype(f32)
        counts = jnp.minimum(position + 1.0, window)
        pooled = (window_sum[RIM:] / counts - rows[RIM:]).astype(bf16)
        mixing = jnp.dot(pooled, pool_weight[g], preferred_element_type=f32)
        act[:, att_w + g * GROUP : att_w + (g + 1) * GROUP] = (
            mixing * pool_scale[:, cols]
        ).astype(bf16)

    lax.fori_loop(2, me + 1, one_step, 0)
    for i in range(heads):
        act[:, i * HEAD : (i + 1) * HEAD] = (acc[i] / sums[i]).astype(bf16)

    for copy in loads:
        copy.wait()

    def block_rows(dx, core):
        first_row = (lax.rem(x + dx, n_x) * 2 + core) * rows_out
        return pl.ds(pl.multiple_of(first_row, 16), rows_out)

    def pair_copy(dx, j):
        return pltpu.make_async_remote_copy(
            src_ref=part.at[j, block_rows(dx, 1 - c)],
            dst_ref=pair_in.at[dx, j],
            send_sem=d_send.at[dx, j],
            recv_sem=d_recv.at[dx, j],
            device_id={"tp": partner},
            device_id_type=MESH,
        )

    def x_copy(dx, j):
        return pltpu.make_async_remote_copy(
            src_ref=x_out.at[dx - 1, j],
            dst_ref=x_in.at[dx - 1, j],
            send_sem=x_send.at[dx - 1, j],
            recv_sem=x_recv.at[dx - 1, j],
            device_id={"tp": across(dx)},
            device_id_type=MESH,
        )

    def to_relay(dx, r):
        return pltpu.make_async_remote_copy(
            src_ref=x_out.at[dx - 1, 2 * r + 1],
            dst_ref=relay_in.at[dx - 1, r],
            send_sem=x_send.at[dx - 1, 2 * r + 1],
            recv_sem=relay_recv.at[dx - 1, r],
            device_id={"sp": relay_at},
            device_id_type=MESH,
        )

    def at_relay(dx, r):
        return pltpu.make_async_remote_copy(
            src_ref=relay_in.at[dx - 1, r],
            dst_ref=relay_mid.at[dx - 1, r],
            send_sem=mid_send.at[dx - 1, r],
            recv_sem=mid_recv.at[dx - 1, r],
            device_id={"tp": across(dx)},
            device_id_type=MESH,
        )

    def from_relay(dx, r):
        return pltpu.make_async_remote_copy(
            src_ref=relay_mid.at[dx - 1, r],
            dst_ref=x_in.at[dx - 1, 2 * r + 1],
            send_sem=back_send.at[dx - 1, r],
            recv_sem=x_recv.at[dx - 1, 2 * r + 1],
            device_id={"sp": n_sp - 1},
            device_id_type=MESH,
        )

    order = list(range(1, n_x)) + [0]

    def project(j):
        part[j] = jnp.dot(act[...], weights[j], preferred_element_type=f32).astype(bf16)
        for dx in order:
            pair_copy(dx, j).start()

    def finish(j):
        for dx in order:
            pair_copy(dx, j).wait_recv()
            total = part[j, block_rows(dx, c)].astype(f32) + pair_in[dx, j].astype(f32)
            if dx == 0:
                own[j] = total
                continue
            x_out[dx - 1, j] = total.astype(bf16)
            detour = jnp.logical_and(
                by_relay, jnp.logical_and(lax.rem(j, 2) == 1, j < 2 * relayed)
            )

            @pl.when(detour)
            def _():
                to_relay(dx, j // 2).start()

            @pl.when(jnp.logical_not(detour))
            def _():
                x_copy(dx, j).start()

    def one_chunk(j, carry):
        project(j)

        @pl.when(j > 0)
        def _():
            finish(j - 1)

        return carry

    lax.fori_loop(0, chunks, one_chunk, 0)
    finish(jnp.int32(chunks - 1))

    def out_copy(j):
        return pltpu.make_async_copy(
            out_buf.at[j],
            out_hbm.at[:, pl.ds(pl.multiple_of(j * CHUNK, CHUNK), CHUNK)],
            out_sems.at[j],
        )

    def last(j, carry):
        total = own[j]
        for dx in range(1, n_x):
            x_copy(dx, j).wait_recv()
            total = total + x_in[dx - 1, j].astype(f32)
        out_buf[j] = total.astype(bf16)
        out_copy(j).start()
        return carry

    lax.fori_loop(0, chunks, last, 0)

    @pl.when(is_relay)
    def _():
        lag = 2
        for r in range(relayed + lag):
            for dx in range(1, n_x):
                if r < relayed:
                    to_relay(dx, r).wait_recv()
                    at_relay(dx, r).start()
                if r >= lag:
                    at_relay(dx, r - lag).wait_recv()
                    from_relay(dx, r - lag).start()
        for r in range(relayed):
            for dx in range(1, n_x):
                at_relay(dx, r).wait_send()
                from_relay(dx, r).wait_send()

    def drain(j, carry):
        out_copy(j).wait()
        for dx in range(n_x):
            pair_copy(dx, j).wait_send()
            if dx:
                x_copy(dx, j).wait_send()
        return carry

    lax.fori_loop(0, chunks, drain, 0)

    @pl.when(has_next)
    def _():
        rim_copy.wait_send()

        def sent(slot, carry):
            for item in range(gate_item + 1):
                hand_on(slot, item).wait_send()
            return carry

        lax.fori_loop(0, me + 1, sent, 0)


def body(n_sp, n_tp, q, k, v, p, gates, q_gain, k_gain, pool_weight, pool_scale, wa, wp):
    length = q.shape[0]
    kv_here = k.shape[1] // HEAD
    heads = kv_here * RATIO
    width = wa.shape[1]
    n_x = n_tp // 2
    rows_out = length // n_tp
    chunks = width // CHUNK
    depth = wa.shape[0] + wp.shape[0]
    items = 2 * kv_here + 1
    dma = pltpu.SemaphoreType.DMA
    hbm = pl.BlockSpec(memory_space=pl.ANY)
    vmem = pl.BlockSpec(memory_space=pltpu.VMEM)
    far = max(n_x - 1, 1)
    return pl.pallas_call(
        functools.partial(kernel, n_sp, n_tp),
        out_shape=jax.ShapeDtypeStruct((rows_out, width), bf16),
        in_specs=[hbm] * 4 + [vmem] * 5 + [hbm] * 2,
        out_specs=hbm,
        scratch_shapes=[
            pltpu.VMEM(q.shape, bf16),
            pltpu.VMEM(k.shape, bf16),
            pltpu.VMEM((n_sp, kv_here, 2, length, HEAD), bf16),
            pltpu.VMEM((n_sp, heads, length), f32),
            pltpu.VMEM((heads, length, 1), f32),
            pltpu.VMEM((heads, length, HEAD), bf16),
            pltpu.VMEM((heads, length, 1), f32),
            pltpu.VMEM((heads, length, 1), f32),
            pltpu.VMEM((heads, length, HEAD), f32),
            pltpu.VMEM((length + RIM, p.shape[1]), bf16),
            pltpu.VMEM((length, depth), bf16),
            pltpu.VMEM((chunks, depth, CHUNK), bf16),
            pltpu.VMEM((chunks, length, CHUNK), bf16),
            pltpu.VMEM((n_x, chunks, rows_out, CHUNK), bf16),
            pltpu.VMEM((far, chunks, rows_out, CHUNK), bf16),
            pltpu.VMEM((far, chunks, rows_out, CHUNK), bf16),
            pltpu.VMEM((chunks, rows_out, CHUNK), f32),
            pltpu.VMEM((chunks, rows_out, CHUNK), bf16),
            pltpu.VMEM((far, max(chunks // 4, 1), rows_out, CHUNK), bf16),
            pltpu.VMEM((far, max(chunks // 4, 1), rows_out, CHUNK), bf16),
            dma((3 + kv_here,)),
            dma((2 * chunks,)),
            dma((n_sp, items)),
            dma((n_sp, items)),
            dma((2,)),
            dma((n_x, chunks)),
            dma((n_x, chunks)),
            dma((far, chunks)),
            dma((far, chunks)),
            dma((far, max(chunks // 4, 1))),
            dma((far, max(chunks // 4, 1))),
            dma((far, max(chunks // 4, 1))),
            dma((far, max(chunks // 4, 1))),
            dma((chunks,)),
        ],
        compiler_params=pltpu.CompilerParams(
            collective_id=0, has_side_effects=True, vmem_limit_bytes=60 * 1024 * 1024
        ),
        name="mixer",
    )(
        q,
        k,
        v,
        p,
        gates.T,
        q_gain.reshape(1, -1),
        k_gain.reshape(1, -1),
        pool_weight,
        pool_scale.reshape(1, -1),
        wa,
        wp,
    )


def solution(mesh):
    return jax.shard_map(
        functools.partial(body, mesh.shape["sp"], mesh.shape["tp"]),
        mesh=mesh,
        in_specs=(
            P(("grp", "sp"), "tp"),
            P(("grp", "sp"), "tp"),
            P(("grp", "sp"), "tp"),
            P(("grp", "sp"), "tp"),
            P(("grp", "sp"), "tp"),
            P(),
            P(),
            P("tp", None, None),
            P("tp"),
            P("tp", None),
            P("tp", None),
        ),
        out_specs=P(("grp", "sp", "tp"), None),
        check_vma=False,
    )
```
